32 devices in a mesh: ep: 8 (over z, x), tp: 4 (over y, core).
Axes of the slice: x: 2, y: 2, z: 4, core: 2. Of those that a mesh axis runs over, the one named last changes fastest.
Arguments:
- x_in: bfloat16 [4096, 3072], P('tp', 'ep'), may hold values from -6 to 6
- z_in: bfloat16 [4096, 3072], P('tp', 'ep'), may hold values from -6 to 6
- dt_raw: float32 [64, 3072], P('tp', 'ep'), may hold values from -6 to 6
- decay_rate: float32 [64], P('tp'), may hold values from 0 to 1, as said below
- b_in: bfloat16 [256, 3072], P(None, 'ep'), may hold values from -6 to 6
- c_in: bfloat16 [256, 3072], P(None, 'ep'), may hold values from -6 to 6
- conv_x: float32 [4096, 4], P('tp'), may hold values from -3 to 3
- conv_b: float32 [256, 4], replicated, may hold values from -3 to 3
- conv_c: float32 [256, 4], replicated, may hold values from -3 to 3
- head_gain: float32 [4096], P('tp'), may hold values from 0.1 to 1.9
- moe_rows: bfloat16 [1280, 2048], P('ep'), may hold values from -6 to 6
- moe_gain: float32 [2048], replicated, may hold values from 0.1 to 1.9
- routes: int32 [1280, 2], P('ep'), may hold values from 0 to 7, all different within a row; in each aligned block of 160 rows (0 to 159, 160 to 319, ...) at most 80 rows name the same one
- route_logit: float32 [1280, 2], P('ep'), may hold values from -6 to 6
- w_gate: bfloat16 [8, 2048, 5120], P('ep', None, 'tp'), may hold values from -0.125 to 0.125
- w_up: bfloat16 [8, 2048, 5120], P('ep', None, 'tp'), may hold values from -0.125 to 0.125
- w_down: bfloat16 [8, 5120, 2048], P('ep', 'tp'), may hold values from -0.078125 to 0.078125
Outputs:
- mixed: bfloat16 [4096, 3072], P('tp', 'ep')
- moe_out: bfloat16 [2048, 1280], P('tp', 'ep')
The draws below stay inside these ranges and needn't reach their ends.
Inputs may be any that keep to these rules, and one draw needn't show every extreme that they name: `routes`: each row names 2 different experts; among the rows of one index of ep no expert is named more than 80 times, a bound that some block reaches. `decay_rate`: positive rates.
All inputs are finite; a program needn't handle non-finite values.
Results may differ from the reference program's by a relative error of at most 0.018.
Values may be sent and summed in bfloat16 or wider, within the bound.
A program may use at most 64 MiB of HBM per device.

```python
import math
import jax
import jax.numpy as jnp
import numpy as np
from jax import lax

D = 2048
HEADS = 64
HEAD_DIM = 64
GROUPS = 2
NSTATE = 128
KCONV = 4
BLOCK = 128
FF = 5120
TOP = 2
L_DEV = 384
MOE_DEV = 160
SEQLEN = 3072
MTOK = 1280
EXPERTS = 8
CAP = 80
N_EP = 8
N_TP = 4


def draw_decay_rate(key, part):
    order_key, slow_key, fast_key = jax.random.split(jax.random.fold_in(key, 11), 3)
    fast_count = HEADS // 2
    is_fast = jax.random.permutation(order_key, HEADS) < fast_count
    slow_rate = jnp.exp(jax.random.uniform(slow_key, (HEADS,), jnp.float32, math.log(0.05 / SEQLEN), math.log(1.0 / SEQLEN)))
    fast_rate = jnp.exp(jax.random.uniform(fast_key, (HEADS,), jnp.float32, math.log(0.012), math.log(0.04)))
    return jnp.where(is_fast, fast_rate, slow_rate)


def draw_dt_raw(key, part):
    noise_key, span_key, block_key = jax.random.split(jax.random.fold_in(key, 23), 3)
    noise = jnp.clip(0.7 * jax.random.normal(noise_key, (HEADS, SEQLEN), jnp.float32), -4.0, 4.0)
    span_shift = jax.random.uniform(span_key, (HEADS, SEQLEN // L_DEV), jnp.float32, -1.5, 1.5)
    block_shift = jax.random.uniform(block_key, (HEADS, SEQLEN // BLOCK), jnp.float32, -0.5, 0.5)
    return noise + jnp.repeat(span_shift, L_DEV, axis=1) + jnp.repeat(block_shift, BLOCK, axis=1)


def levels(stream_key, extent, pieces, smallest, largest):
    loudness, own = 1.0, jax.random.fold_in(stream_key, 6)
    for axis_at, shards_of in pieces:
        steps = jnp.exp(jax.random.uniform(jax.random.fold_in(own, axis_at), (shards_of,), jnp.float32, smallest / len(pieces), largest / len(pieces)))
        loudness = loudness * jnp.repeat(steps, extent[axis_at] // shards_of).reshape([-1 if axis == axis_at else 1 for axis in range(len(extent))])
    return loudness


def assign_block(stream_key, own, number, rows, amount, top, bound, lean):
    ranking = jax.random.permutation(stream_key, amount)
    crowded, usual = portions_of(amount, rows * top, bound, lean, True), portions_of(amount, rows * top, bound, lean, False)
    places = jnp.arange(amount)

    def named(sizes, rotation):
        used = int((sizes > 0).sum())
        fixed = max(1, used // 4)
        moved = fixed + (places - fixed + rotation * (used - fixed)) % max(1, amount - fixed)
        return jnp.zeros((amount,), jnp.int32).at[ranking[jnp.where(places < fixed, places, moved)]].set(jnp.asarray(sizes, jnp.int32))

    sizes = jnp.where(number % 4 == 0, named(crowded, number // 4), named(usual, number - number // 4 - 1))
    mixed = jax.random.permutation(jax.random.fold_in(own, 3), amount)
    giver, receiver = mixed[0:amount // 2 * 2:2], mixed[1:amount // 2 * 2:2]
    slack = jnp.minimum(sizes[giver] - 1, bound - sizes[receiver]) // 2
    slack = jnp.where((giver == ranking[0]) | (receiver == ranking[0]) | (sizes[receiver] == 0), 0, jnp.maximum(slack, 0))
    moved = jax.random.randint(jax.random.fold_in(own, 4), (amount // 2,), 0, 1 << 20) % (slack + 1)
    sizes = sizes.at[giver].add(-moved).at[receiver].add(moved)
    items = jnp.searchsorted(jnp.cumsum(sizes), jnp.arange(rows * top), side="right").astype(jnp.int32)
    grid = items.reshape(top, rows).T
    grid = grid[jax.random.permutation(jax.random.fold_in(own, 1), rows)]
    rotation = jax.random.randint(jax.random.fold_in(own, 2), (rows, 1), 0, top)
    return jnp.take_along_axis(grid, (jnp.arange(top)[None, :] + rotation) % top, axis=1)


def portions_of(amount, total, most, skew, full):
    loads = [(1 << 20) // math.isqrt(grade ** skew) + 1 for grade in range(1, amount + 1)]
    largest = most if full else min(most, max(-(-total // amount), total * loads[0] // sum(loads)))
    least = 1 if total - largest >= amount - 1 else 0
    given, spare = [largest] + [least] * (amount - 1), total - largest - least * (amount - 1)
    while spare > 0:
        free = [i for i in range(1, amount) if given[i] < largest] or [i for i in range(1, amount) if given[i] < most]
        mass, left = sum([loads[i] for i in free]), spare
        for i in free:
            addition = min(most - given[i], max(1, left * loads[i] // mass), spare)
            given[i] = given[i] + addition
            spare = spare - addition
    return np.array(given)


def gaussian(own_key, dims, width, reach, shards=(), held_as=jnp.bfloat16):
    values = width * jax.random.normal(own_key, dims, jnp.float32)
    if shards:
        values = values * levels(own_key, dims, shards, -0.22, 0.18)
    return jnp.clip(values, -reach, reach).astype(held_as)


def setup_inputs(seed: int = 0) -> dict:
    key_of = jax.random.split(jax.random.key(seed), 18)
    x_in = gaussian(key_of[0], (HEADS * HEAD_DIM, SEQLEN), 1.0, 6.0, ((0, 4), (1, 8)))
    z_in = gaussian(key_of[1], (HEADS * HEAD_DIM, SEQLEN), 1.0, 6.0, ((0, 4), (1, 8)))
    dt_raw = draw_dt_raw(jax.random.fold_in(key_of[17], 71), 0)
    decay_rate = draw_decay_rate(jax.random.fold_in(key_of[17], 71), 0)
    b_in = gaussian(key_of[4], (GROUPS * NSTATE, SEQLEN), 1.0, 6.0, ((1, 8),))
    c_in = gaussian(key_of[5], (GROUPS * NSTATE, SEQLEN), 1.0, 6.0, ((1, 8),))
    conv_x = gaussian(key_of[6], (HEADS * HEAD_DIM, KCONV), KCONV ** -0.5, 3.0, ((0, 4),), jnp.float32)
    conv_b = gaussian(key_of[7], (GROUPS * NSTATE, KCONV), KCONV ** -0.5, 3.0, (), jnp.float32)
    conv_c = gaussian(key_of[8], (GROUPS * NSTATE, KCONV), KCONV ** -0.5, 3.0, (), jnp.float32)
    head_gain = jnp.clip(1.0 + 0.18 * jax.random.normal(key_of[9], (HEADS * HEAD_DIM,), jnp.float32), 0.1, 1.9)
    moe_rows = gaussian(key_of[10], (MTOK, D), 1.0, 6.0, ((0, 8),))
    moe_gain = jnp.clip(1.0 + 0.18 * jax.random.normal(key_of[11], (D,), jnp.float32), 0.1, 1.9)
    routes_keys = jax.random.split(jax.random.fold_in(key_of[12], 1), MTOK // MOE_DEV)
    routes_turns = jax.random.permutation(jax.random.fold_in(key_of[12], 3), MTOK // MOE_DEV)
    routes = jax.vmap(lambda own, number: assign_block(jax.random.fold_in(key_of[12], 2), own, number, MOE_DEV, EXPERTS, TOP, CAP, 2))(routes_keys, routes_turns).reshape((MTOK, TOP))
    route_logit = gaussian(key_of[13], (MTOK, TOP), 1.5, 6.0, ((0, 8),), jnp.float32)
    w_gate = gaussian(key_of[14], (EXPERTS, D, FF), D ** -0.5, 0.125, ((0, 8), (2, 4)))
    w_up = gaussian(key_of[15], (EXPERTS, D, FF), D ** -0.5, 0.125, ((0, 8), (2, 4)))
    w_down = gaussian(key_of[16], (EXPERTS, FF, D), FF ** -0.5, 0.078125, ((0, 8), (1, 4)))
    return dict(x_in=x_in, z_in=z_in, dt_raw=dt_raw, decay_rate=decay_rate, b_in=b_in, c_in=c_in, conv_x=conv_x, conv_b=conv_b, conv_c=conv_c, head_gain=head_gain, moe_rows=moe_rows, moe_gain=moe_gain, routes=routes, route_logit=route_logit, w_gate=w_gate, w_up=w_up, w_down=w_down)


HIGHEST = lax.Precision.HIGHEST
ROW_EPS = 0.1
HEAD_EPS = 1.0

def causal_conv(signal, weight):
    taps = weight.shape[1]
    length = signal.shape[1]
    padded = jnp.pad(signal, ((0, 0), (taps - 1, 0)))
    running = jnp.zeros(signal.shape, jnp.float32)
    for offset in range(taps):
        running = running + weight[:, offset:offset + 1] * padded[:, offset:offset + length]
    return jax.nn.silu(running)

def block_step(state_in, x_block, b_block, c_block, log_block, step_block):
    cum_log = jnp.cumsum(log_block, axis=1)
    seg_log = cum_log[:, :, None] - cum_log[:, None, :]
    causal = jnp.tril(jnp.ones((log_block.shape[1], log_block.shape[1]), bool))
    decay_mask = jnp.exp(jnp.where(causal[None], seg_log, -jnp.inf))
    scores = jnp.einsum('hnt,hns->hts', c_block, b_block, precision=HIGHEST) * decay_mask * step_block[:, None, :]
    inner_term = jnp.einsum('hts,hps->hpt', scores, x_block, precision=HIGHEST)
    carried = jnp.einsum('hnt,hpn->hpt', c_block, state_in, precision=HIGHEST) * jnp.exp(cum_log)[:, None, :]
    tail_weight = jnp.exp(cum_log[:, -1:] - cum_log) * step_block
    fresh_state = jnp.einsum('hps,hns->hpn', x_block * tail_weight[:, None, :], b_block, precision=HIGHEST)
    new_state = jnp.exp(cum_log[:, -1])[:, None, None] * state_in + fresh_state
    return (new_state, inner_term + carried)

def mixer_half(x_in, z_in, dt_raw, decay_rate, b_in, c_in, conv_x, conv_b, conv_c, head_gain):
    x_conv = causal_conv(x_in.astype(jnp.float32), conv_x.astype(jnp.float32)).reshape(HEADS, HEAD_DIM, SEQLEN)
    b_conv = causal_conv(b_in.astype(jnp.float32), conv_b.astype(jnp.float32)).reshape(GROUPS, NSTATE, SEQLEN)
    c_conv = causal_conv(c_in.astype(jnp.float32), conv_c.astype(jnp.float32)).reshape(GROUPS, NSTATE, SEQLEN)
    step_dt = jax.nn.softplus(dt_raw.astype(jnp.float32))
    log_decay = -step_dt * decay_rate.astype(jnp.float32)[:, None]
    block_count = SEQLEN // BLOCK
    per_group = HEADS // GROUPS

    def blocks(tensor):
        return jnp.moveaxis(tensor.reshape(tensor.shape[:-1] + (block_count, BLOCK)), -2, 0)

    def advance(state_in, inputs):
        x_block, b_block, c_block, log_block, step_block = inputs
        return block_step(state_in, x_block, jnp.repeat(b_block, per_group, axis=0), jnp.repeat(c_block, per_group, axis=0), log_block, step_block)
    init_state = jnp.zeros((HEADS, HEAD_DIM, NSTATE), jnp.float32)
    _, block_out = lax.scan(advance, init_state, (blocks(x_conv), blocks(b_conv), blocks(c_conv), blocks(log_decay), blocks(step_dt)))
    y_mixed = jnp.moveaxis(block_out, 0, -2).reshape(HEADS, HEAD_DIM, SEQLEN)
    gated_out = y_mixed * jax.nn.silu(z_in.astype(jnp.float32).reshape(HEADS, HEAD_DIM, SEQLEN))
    head_scale = lax.rsqrt(lax.optimization_barrier(jnp.mean(gated_out * gated_out, axis=1, keepdims=True)) + HEAD_EPS)
    normed_out = gated_out * head_scale * head_gain.astype(jnp.float32).reshape(HEADS, HEAD_DIM, 1)
    return normed_out.reshape(HEADS * HEAD_DIM, SEQLEN).astype(jnp.bfloat16)

def experts_half(moe_rows, moe_gain, routes, route_logit, w_gate, w_up, w_down):
    rows_float = moe_rows.astype(jnp.float32)
    row_scale = lax.rsqrt(lax.optimization_barrier(jnp.mean(rows_float * rows_float, axis=1, keepdims=True)) + ROW_EPS)
    normed = (rows_float * row_scale * moe_gain.astype(jnp.float32)).astype(jnp.bfloat16)
    by_source = routes.reshape(N_EP, MOE_DEV * TOP)
    hit_table = (by_source[:, :, None] == jnp.arange(EXPERTS, dtype=jnp.int32)).astype(jnp.int32)
    slot_rank = lax.optimization_barrier(jnp.sum((jnp.cumsum(hit_table, axis=1) - hit_table) * hit_table, axis=2))
    slot_index = (jnp.arange(N_EP, dtype=jnp.int32)[:, None] * CAP + slot_rank).reshape(-1).astype(jnp.int32)
    expert_index = routes.reshape(-1).astype(jnp.int32)
    token_index = (jnp.arange(MTOK * TOP, dtype=jnp.int32) // TOP).astype(jnp.int32)
    buffer = jnp.zeros((EXPERTS, N_EP * CAP, D), jnp.bfloat16).at[expert_index, slot_index].set(normed[token_index])
    block_width = FF // N_TP

    def run_expert(inputs):
        rows_in, gate_weight, up_weight, down_weight = inputs
        gate_act = jnp.dot(rows_in, gate_weight, preferred_element_type=jnp.float32)
        up_act = jnp.dot(rows_in, up_weight, preferred_element_type=jnp.float32)
        hidden = (jax.nn.silu(gate_act) * up_act).astype(jnp.bfloat16)
        running = jnp.zeros((rows_in.shape[0], D), jnp.float32)
        for part_index in range(N_TP):
            lower = part_index * block_width
            piece_sum = jnp.dot(hidden[:, lower:lower + block_width], down_weight[lower:lower + block_width], preferred_element_type=jnp.float32)
            running = running + lax.optimization_barrier(piece_sum.astype(jnp.bfloat16)).astype(jnp.float32)
        return running.astype(jnp.bfloat16)
    results = lax.map(run_expert, (buffer, w_gate, w_up, w_down))
    picked = results[expert_index, slot_index].astype(jnp.float32).reshape(MTOK, TOP, D)
    weight = jax.nn.sigmoid(route_logit - route_logit[:, ::-1])
    combined = lax.optimization_barrier(jnp.sum(picked * weight[:, :, None], axis=1))
    return combined.T.astype(jnp.bfloat16)

def reference(x_in, z_in, dt_raw, decay_rate, b_in, c_in, conv_x, conv_b, conv_c, head_gain, moe_rows, moe_gain, routes, route_logit, w_gate, w_up, w_down):
    mixed = mixer_half(x_in, z_in, dt_raw, decay_rate, b_in, c_in, conv_x, conv_b, conv_c, head_gain)
    moe_out = experts_half(moe_rows, moe_gain, routes, route_logit, w_gate, w_up, w_down)
    return (mixed, moe_out)
```

```python
import functools
import jax
import jax.numpy as jnp
from jax import lax
from jax.experimental import pallas as pl
from jax.experimental.pallas import tpu as pltpu
from jax.sharding import PartitionSpec as P

HEADS = 64
HEAD_DIM = 64
GROUPS = 2
NSTATE = 128
BLOCK = 128
ROW_EPS = 0.1
HEAD_EPS = 1.0
LANES = 128
F32 = jnp.float32
BF16 = jnp.bfloat16
VMEM = pltpu.VMEM


def vmem_specs(count):
    return [pl.BlockSpec(memory_space=VMEM)] * count


def cost(flops, moved):
    return pl.CostEstimate(flops=flops, bytes_accessed=moved, transcendentals=0)


def dot(a, b, dims, precision=None):
    return lax.dot_general(a, b, (dims, ((), ())), preferred_element_type=F32, precision=precision)


def silu(v):
    return v / (1.0 + jnp.exp(-v))


def conv_rows(signal, rim, weight):
    taps = weight.shape[1]
    joined = jnp.concatenate([rim.astype(F32), signal.astype(F32)], axis=1)
    running = weight[:, taps - 1 : taps] * joined[:, LANES:]
    for back in range(1, taps):
        moved = pltpu.roll(joined, back, 1)[:, LANES:]
        running = running + weight[:, taps - 1 - back : taps - back] * moved
    return silu(running)


def prefix_decays(dt_ref, rate_ref):
    dt = dt_ref[...]
    step = jnp.maximum(dt, 0.0) + jnp.log1p(jnp.exp(-jnp.abs(dt)))
    log_decay = -step * rate_ref[...]
    length = dt.shape[1]
    row = lax.broadcasted_iota(jnp.int32, (length, length), 0)
    col = lax.broadcasted_iota(jnp.int32, (length, length), 1)
    upper = jnp.where(row <= col, 1.0, 0.0).astype(F32)
    lower = jnp.where(row >= col, 1.0, 0.0).astype(F32)
    high = lax.Precision.HIGHEST
    cum = dot(log_decay, upper, ((1,), (0,)), high)
    cum_col = dot(lower, log_decay, ((1,), (1,)), high)
    return step, cum, cum_col


def span_kernel(
    x_ref, rim_ref, tapx_ref, b_ref, brim_ref, tapb_ref, c_ref, crim_ref, tapc_ref, dt_ref, rate_ref,
    y_ref, state_ref, conv_ref, cum_ref, reach_ref, step_ref, col_ref, score_ref, bconv_ref,
):
    heads, length = dt_ref.shape
    step, cum, cum_col = prefix_decays(dt_ref, rate_ref)
    step_ref[...] = step
    cum_ref[...] = cum
    reach_ref[...] = jnp.exp(cum[:, length - 1 :])
    b_conv = conv_rows(b_ref[...], brim_ref[...], tapb_ref[...]).astype(BF16)
    c_conv = conv_rows(c_ref[...], crim_ref[...], tapc_ref[...]).astype(BF16)
    bconv_ref[...] = b_conv
    conv_ref[...] = c_conv
    score_ref[...] = dot(b_conv, c_conv, ((0,), (0,)))
    row = lax.broadcasted_iota(jnp.int32, (BLOCK, BLOCK), 0)
    col = lax.broadcasted_iota(jnp.int32, (BLOCK, BLOCK), 1)
    causal = row <= col
    for head in range(heads):
        col_ref[head] = jnp.broadcast_to(cum_col[:, head : head + 1], (length, LANES))

    def one(head, carry):
        rows = pl.ds(pl.multiple_of(head * HEAD_DIM, HEAD_DIM), HEAD_DIM)
        x = conv_rows(x_ref[rows, :], rim_ref[rows, :], tapx_ref[rows, :])
        own = cum_ref[pl.ds(head, 1), :]
        xs = x * step_ref[pl.ds(head, 1), :]
        tail = xs * jnp.exp(own[:, length - 1 :] - own)
        state_ref[rows, :] = dot(tail.astype(BF16), bconv_ref[...], ((1,), (1,)))
        xs = xs.astype(BF16)
        for target in range(length // BLOCK):
            at = slice(target * BLOCK, (target + 1) * BLOCK)
            pieces = []
            for source in range(target + 1):
                of = slice(source * BLOCK, (source + 1) * BLOCK)
                gap = own[:, at] - col_ref[head, of, :]
                if source == target:
                    gap = jnp.where(causal, gap, -jnp.inf)
                pieces.append((score_ref[of, at] * jnp.exp(gap)).astype(BF16))
            mask = pieces[0] if target == 0 else jnp.concatenate(pieces, axis=0)
            y_ref[rows, at] = dot(xs[:, : (target + 1) * BLOCK], mask, ((1,), (0,)))
        return carry

    lax.fori_loop(0, heads, one, 0)


def close_kernel(y_ref, state_ref, conv_ref, cum_ref, z_ref, gain_ref, out_ref):
    heads = cum_ref.shape[0]

    def one(head, carry):
        rows = pl.ds(pl.multiple_of(head * HEAD_DIM, HEAD_DIM), HEAD_DIM)
        carried = dot(state_ref[rows, :].astype(BF16), conv_ref[...], ((1,), (0,)))
        y = y_ref[rows, :] + carried * jnp.exp(cum_ref[pl.ds(head, 1), :])
        gated = y * silu(z_ref[rows, :].astype(F32))
        scale = lax.rsqrt(jnp.mean(gated * gated, axis=0, keepdims=True) + HEAD_EPS)
        out_ref[rows, :] = (gated * scale * gain_ref[rows, :]).astype(BF16)
        return carry

    lax.fori_loop(0, heads, one, 0)


def outbox_kernel(rows_ref, gain_ref, routes_ref, logit_ref, out_ref, pick_ref, *, experts, capacity):
    width = out_ref.shape[1]
    tokens = rows_ref.shape[0]
    values = rows_ref[...].astype(F32)
    scale = lax.rsqrt(jnp.mean(values * values, axis=1, keepdims=True) + ROW_EPS)
    column = pl.ds(pl.multiple_of(lax.axis_index("tp") * width, LANES), width)
    normed = (rows_ref[:, column].astype(F32) * scale * gain_ref[:, column]).astype(BF16)
    routes = routes_ref[...]
    logit = logit_ref[...]
    first = 1.0 / (1.0 + jnp.exp(logit[1:2] - logit[0:1]))
    second = 1.0 / (1.0 + jnp.exp(logit[0:1] - logit[1:2]))
    number = lax.broadcasted_iota(jnp.int32, (experts, tokens), 0)
    in_first = number == routes[0:1]
    in_second = number == routes[1:2]
    hits = jnp.where(in_first, 1.0, 0.0) + jnp.where(in_second, 1.0, 0.0)
    row = lax.broadcasted_iota(jnp.int32, (tokens, tokens), 0)
    col = lax.broadcasted_iota(jnp.int32, (tokens, tokens), 1)
    earlier = jnp.where(row < col, 1.0, 0.0).astype(BF16)
    rank = dot(hits.astype(BF16), earlier, ((1,), (0,)))
    weight = jnp.where(in_first, first, 0.0) + jnp.where(in_second, second, 0.0)
    slot = jnp.where(hits > 0.0, number * capacity + rank.astype(jnp.int32), -1)
    place = lax.broadcasted_iota(jnp.int32, (experts * capacity, tokens), 0)
    chosen = jnp.zeros((experts * capacity, tokens), F32)
    weighed = jnp.zeros((experts * capacity, tokens), F32)
    for expert in range(experts):
        same = place == slot[expert : expert + 1]
        chosen = jnp.where(same, 1.0, chosen)
        weighed = jnp.where(same, weight[expert : expert + 1], weighed)
    pick_ref[...] = weighed.astype(BF16)
    out_ref[...] = dot(chosen.astype(BF16), normed, ((1,), (0,))).astype(BF16)


def ffn_kernel(parts, *refs):
    pieces = refs[:parts]
    gate_ref, up_ref, down_ref = refs[parts : parts + 3]
    outs = refs[parts + 3 : 2 * parts + 3]
    joined, total = refs[2 * parts + 3 :]
    me = lax.axis_index("tp")
    width = pieces[0].shape[1]
    turn = pl.program_id(0)

    def column(part):
        return pl.ds(pl.multiple_of((me ^ part) * width, LANES), width)

    @pl.when(turn == 0)
    def _():
        for part in range(parts):
            joined[:, column(part)] = pieces[part][...]

    gate = dot(joined[...], gate_ref[0], ((1,), (0,)))
    up = dot(joined[...], up_ref[0], ((1,), (0,)))
    hidden = (silu(gate) * up).astype(BF16)
    partial = dot(hidden, down_ref[0], ((1,), (0,)))

    @pl.when(turn == 0)
    def _():
        total[...] = partial

    @pl.when(turn > 0)
    def _():
        total[...] += partial

    @pl.when(turn == pl.num_programs(0) - 1)
    def _():
        for part in range(parts):
            outs[part][...] = total[:, column(part)].astype(BF16)


def combine_kernel(back_ref, pick_ref, out_ref):
    out_ref[...] = dot(back_ref[...], pick_ref[...], ((0,), (0,))).astype(BF16)


def from_behind(value, axis, steps):
    count = lax.axis_size(axis)
    return lax.ppermute(value, axis, [(source, source + steps) for source in range(count - steps)])


def swap(value, axis, bit):
    count = lax.axis_size(axis)
    return lax.ppermute(value, axis, [(source, source ^ bit) for source in range(count)])


def on_device(
    x_in, z_in, dt_raw, decay_rate, b_in, c_in, conv_x, conv_b, conv_c, head_gain,
    moe_rows, moe_gain, routes, route_logit, w_gate, w_up, w_down,
):
    heads, length = dt_raw.shape
    value_rows = x_in.shape[0]
    taps = conv_x.shape[1]
    tp_size = lax.axis_size("tp")
    ep_size = lax.axis_size("ep")
    tokens, features = moe_rows.shape
    top = routes.shape[1]
    experts = ep_size
    capacity = 2 * tokens * top // experts
    width = features // tp_size
    slots = experts * capacity

    outbox, pick = pl.pallas_call(
        functools.partial(outbox_kernel, experts=experts, capacity=capacity),
        out_shape=(
            jax.ShapeDtypeStruct((slots, width), BF16),
            jax.ShapeDtypeStruct((slots, tokens), BF16),
        ),
        in_specs=vmem_specs(4),
        out_specs=tuple(vmem_specs(2)),
        name="outbox",
        cost_estimate=cost(2 * slots * tokens * width, 2 * tokens * features),
    )(moe_rows, moe_gain.reshape(1, features), routes.T, route_logit.T)
    arrived = lax.all_to_all(
        outbox.reshape(experts, capacity, width), "ep", split_axis=0, concat_axis=0, tiled=True
    ).reshape(slots, width)

    group = lax.axis_index("tp") * heads // (HEADS // GROUPS)

    def of_group(tensor):
        return lax.dynamic_slice_in_dim(tensor, group * NSTATE, NSTATE, 0)

    b_own, c_own, taps_b, taps_c = map(of_group, (b_in, c_in, conv_b, conv_c))
    edge = length - taps + 1
    ends = jnp.concatenate([x_in[:, edge:], b_own[:, edge:], c_own[:, edge:]], axis=0)
    rims = from_behind(ends.T, "ep", 1).T
    rims = jnp.pad(rims, ((0, 0), (LANES - taps + 1, 0)))
    y_local, state, c_conv, cum, reach = pl.pallas_call(
        span_kernel,
        out_shape=(
            jax.ShapeDtypeStruct((value_rows, length), F32),
            jax.ShapeDtypeStruct((value_rows, NSTATE), F32),
            jax.ShapeDtypeStruct((NSTATE, length), BF16),
            jax.ShapeDtypeStruct((heads, length), F32),
            jax.ShapeDtypeStruct((heads, 1), F32),
        ),
        in_specs=vmem_specs(11),
        out_specs=tuple(vmem_specs(5)),
        scratch_shapes=[
            VMEM((heads, length), F32),
            VMEM((heads, length, LANES), F32),
            VMEM((length, length), F32),
            VMEM((NSTATE, length), BF16),
        ],
        name="span",
        cost_estimate=cost(10**10, 4 * 10**6),
    )(
        x_in, rims[:value_rows], conv_x,
        b_own, rims[value_rows : value_rows + NSTATE], taps_b,
        c_own, rims[value_rows + NSTATE :], taps_c,
        dt_raw, decay_rate.reshape(heads, 1),
    )

    def passed(state, reach, steps):
        moved = from_behind(state.astype(BF16), "ep", steps).astype(F32)
        return moved, from_behind(reach, "ep", steps)

    state, reach = passed(state.reshape(heads, HEAD_DIM, NSTATE), reach, 1)
    steps = 1
    while steps < ep_size - 1:
        before, before_reach = passed(state, reach, steps)
        state = state + reach[:, :, None] * before
        reach = reach * before_reach
        steps *= 2
    incoming = state.reshape(value_rows, NSTATE).astype(BF16)

    parts = {0: arrived}
    bit = tp_size // 2
    while bit:
        parts.update({part | bit: swap(parts[part], "tp", bit) for part in list(parts)})
        bit //= 2
    hidden_units = w_gate.shape[2]
    tile = 256 if hidden_units % 256 == 0 else hidden_units if hidden_units % LANES else LANES
    if hidden_units < 1024:
        tile = hidden_units
    outs = pl.pallas_call(
        functools.partial(ffn_kernel, tp_size),
        grid=(hidden_units // tile,),
        out_shape=[jax.ShapeDtypeStruct((slots, width), BF16)] * tp_size,
        in_specs=vmem_specs(tp_size)
        + [
            pl.BlockSpec((1, features, tile), lambda i: (0, 0, i)),
            pl.BlockSpec((1, features, tile), lambda i: (0, 0, i)),
            pl.BlockSpec((1, tile, features), lambda i: (0, i, 0)),
        ],
        out_specs=vmem_specs(tp_size),
        scratch_shapes=[VMEM((slots, features), BF16), VMEM((slots, features), F32)],
        compiler_params=pltpu.CompilerParams(dimension_semantics=("arbitrary",), vmem_limit_bytes=56 * 2**20),
        name="ffn",
        cost_estimate=cost(6 * slots * features * hidden_units, 6 * features * hidden_units),
    )(*[parts[part] for part in range(tp_size)], w_gate, w_up, w_down)
    sums = dict(enumerate(outs))
    bit = 1
    while bit < tp_size:
        received = {part: swap(sums[part], "tp", bit) for part in sums if part & bit}
        sums = {
            part: (sums[part].astype(F32) + received[part | bit].astype(F32)).astype(BF16)
            for part in sums
            if not part & bit
        }
        bit *= 2
    returned = lax.all_to_all(
        sums[0].reshape(experts, capacity, width), "ep", split_axis=0, concat_axis=0, tiled=True
    ).reshape(slots, width)

    mixed = pl.pallas_call(
        close_kernel,
        out_shape=jax.ShapeDtypeStruct((value_rows, length), BF16),
        in_specs=vmem_specs(6),
        out_specs=pl.BlockSpec(memory_space=VMEM),
        name="close",
        cost_estimate=cost(4 * 10**9, 4 * 10**6),
    )(y_local, incoming, c_conv, cum, z_in, head_gain.reshape(value_rows, 1))
    moe_out = pl.pallas_call(
        combine_kernel,
        out_shape=jax.ShapeDtypeStruct((width, tokens), BF16),
        in_specs=vmem_specs(2),
        out_specs=pl.BlockSpec(memory_space=VMEM),
        name="combine",
        cost_estimate=cost(2 * slots * tokens * width, 2 * slots * width),
    )(returned, pick)
    return (mixed, moe_out)


def solution(mesh):
    return jax.shard_map(
        on_device,
        mesh=mesh,
        in_specs=(
            P("tp", "ep"), P("tp", "ep"), P("tp", "ep"), P("tp"), P(None, "ep"), P(None, "ep"),
            P("tp", None), P(), P(), P("tp"), P("ep", None), P(), P("ep", None), P("ep", None),
            P("ep", None, "tp"), P("ep", None, "tp"), P("ep", "tp", None),
        ),
        out_specs=(P("tp", "ep"), P("tp", "ep")),
        check_vma=False,
    )
```

```python
import functools
import jax
import jax.numpy as jnp
from jax import lax
from jax.experimental import pallas as pl
from jax.experimental.pallas import tpu as pltpu
from jax.sharding import PartitionSpec as P

HEADS = 64
HEAD_DIM = 64
GROUPS = 2
NSTATE = 128
BLOCK = 128
ROW_EPS = 0.1
HEAD_EPS = 1.0
LANES = 128
F32 = jnp.float32
BF16 = jnp.bfloat16
VMEM = pltpu.VMEM
MESH = pl.DeviceIdType.MESH


def vmem_specs(count):
    return [pl.BlockSpec(memory_space=VMEM)] * count


def cost(flops, moved):
    return pl.CostEstimate(flops=flops, bytes_accessed=moved, transcendentals=0)


def dot(a, b, dims, precision=None):
    return lax.dot_general(a, b, (dims, ((), ())), preferred_element_type=F32, precision=precision)


def eye(count):
    row = lax.broadcasted_iota(jnp.int32, (count, count), 0)
    col = lax.broadcasted_iota(jnp.int32, (count, count), 1)
    return jnp.where(row == col, 1.0, 0.0).astype(F32)


def upright(flat):
    return dot(flat, eye(flat.shape[0]), ((0,), (0,)), lax.Precision.HIGHEST)


def silu(v):
    return v / (1.0 + jnp.exp(-v))


def conv_rows(signal, rim, weight):
    taps = weight.shape[1]
    joined = jnp.concatenate([rim.astype(F32), signal.astype(F32)], axis=1)
    running = weight[:, taps - 1 : taps] * joined[:, LANES:]
    for back in range(1, taps):
        moved = pltpu.roll(joined, back, 1)[:, LANES:]
        running = running + weight[:, taps - 1 - back : taps - back] * moved
    return silu(running)


def prefix_decays(dt_ref, rate_ref):
    dt = dt_ref[...]
    step = jnp.maximum(dt, 0.0) + jnp.log1p(jnp.exp(-jnp.abs(dt)))
    rate = jnp.where(eye(dt.shape[0]) > 0.0, rate_ref[...], 0.0)
    log_decay = -step * jnp.sum(rate, axis=1, keepdims=True)
    length = dt.shape[1]
    row = lax.broadcasted_iota(jnp.int32, (length, length), 0)
    col = lax.broadcasted_iota(jnp.int32, (length, length), 1)
    upper = jnp.where(row <= col, 1.0, 0.0).astype(F32)
    lower = jnp.where(row >= col, 1.0, 0.0).astype(F32)
    high = lax.Precision.HIGHEST
    cum = dot(log_decay, upper, ((1,), (0,)), high)
    cum_col = dot(lower, log_decay, ((1,), (1,)), high)
    return step, cum, cum_col


def flip(place, mask):
    bit = 1
    while bit <= mask:
        if mask & bit:
            place = place + bit * (1 - 2 * ((place // bit) % 2))
        bit *= 2
    return place


def greet(ep_size, tp_size):
    barrier = pltpu.get_barrier_semaphore()
    me, lane = lax.axis_index("ep"), lax.axis_index("tp")
    count = 0
    for hop in range(1, ep_size):
        pl.semaphore_signal(barrier, 1, device_id={"ep": (me + hop) % ep_size}, device_id_type=MESH)
        count += 1
    bit = 1
    while bit < tp_size:
        pl.semaphore_signal(barrier, 1, device_id={"tp": flip(lane, bit)}, device_id_type=MESH)
        count += 1
        bit *= 2
    pl.semaphore_wait(barrier, count)


def remote(source, target, send, recv, **where):
    return pltpu.make_async_remote_copy(
        src_ref=source, dst_ref=target, send_sem=send, recv_sem=recv, device_id=where, device_id_type=MESH
    )


class Prefix:
    def __init__(self, state, reach, out, out_reach, got, got_reach, send, recv, ep_size):
        self.state, self.reach = state, reach
        self.out, self.out_reach, self.got, self.got_reach = out, out_reach, got, got_reach
        self.send, self.recv, self.size = send, recv, ep_size

    def copies(self, turn, steps):
        target = (lax.axis_index("ep") + steps) % self.size
        return (
            remote(self.out.at[turn], self.got.at[turn], self.send.at[turn, 0], self.recv.at[turn, 0], ep=target),
            remote(self.out_reach.at[turn], self.got_reach.at[turn], self.send.at[turn, 1], self.recv.at[turn, 1], ep=target),
        )

    def begin(self, turn, steps):
        me = lax.axis_index("ep")

        @pl.when(me + steps < self.size)
        def _():
            self.out[turn] = self.state[...].astype(BF16)
            self.out_reach[turn] = self.reach[...]
            for copy in self.copies(turn, steps):
                copy.start()

    def finish(self, turn, steps, first):
        me = lax.axis_index("ep")

        @pl.when(me >= steps)
        def _():
            for copy in self.copies(turn, steps):
                copy.wait_recv()
            if first:
                self.state[...] = self.got[turn].astype(F32)
                self.reach[...] = self.got_reach[turn]
            else:
                for head in range(self.reach.shape[0]):
                    rows = slice(head * HEAD_DIM, (head + 1) * HEAD_DIM)
                    before = self.got[turn, rows, :].astype(F32)
                    self.state[rows, :] = self.state[rows, :] + self.reach[head : head + 1, :] * before
                self.reach[...] = self.reach[...] * self.got_reach[turn]

        if first:

            @pl.when(me < steps)
            def _():
                self.state[...] = jnp.zeros_like(self.state)
                self.reach[...] = jnp.zeros_like(self.reach)

        @pl.when(me + steps < self.size)
        def _():
            for copy in self.copies(turn, steps):
                copy.wait_send()


def spread_kernel(
    rows_ref, gain_ref, routes_ref, logit_ref, x_ref, tapx_ref, b_ref, tapb_ref, c_ref, tapc_ref, dt_ref, rate_ref,
    joined_ref, pick_ref, y_ref, state_ref, reach_ref, conv_ref, cum_ref,
    outbox, rank_ref, weight_ref, xrim, brim, crim, tap_col, tapb_col, tapc_col,
    step_ref, col_ref, score_ref, bconv_ref, out, out_reach, got, got_reach,
    rim_send, rim_recv, box_send, box_recv, ag_send, ag_recv, pre_send, pre_recv,
    *, ep_size, tp_size,
):
    me, lane = lax.axis_index("ep"), lax.axis_index("tp")
    experts, capacity, features = joined_ref.shape
    width = features // tp_size
    tokens = rows_ref.shape[0]
    heads, length = dt_ref.shape

    def cols(part):
        return pl.ds(pl.multiple_of(flip(lane, part) * width, LANES), width)

    greet(ep_size, tp_size)
    end = pl.ds(length - LANES, LANES)
    after = (me + 1) % ep_size
    rims = [
        remote(source.at[:, end], target, rim_send.at[i], rim_recv.at[i], ep=after)
        for i, (source, target) in enumerate(((x_ref, xrim), (b_ref, brim), (c_ref, crim)))
    ]

    @pl.when(me + 1 < ep_size)
    def _():
        for copy in rims:
            copy.start()

    @pl.when(me == 0)
    def _():
        for ref in (xrim, brim, crim):
            ref[...] = jnp.zeros_like(ref)

    values = rows_ref[...].astype(F32)
    scale = lax.rsqrt(jnp.mean(values * values, axis=1, keepdims=True) + ROW_EPS)
    normed = (rows_ref[:, cols(0)].astype(F32) * scale * gain_ref[:, cols(0)]).astype(BF16)
    routes = routes_ref[...]
    logit = logit_ref[...]
    first = 1.0 / (1.0 + jnp.exp(logit[1:2] - logit[0:1]))
    second = 1.0 / (1.0 + jnp.exp(logit[0:1] - logit[1:2]))
    number = lax.broadcasted_iota(jnp.int32, (experts, tokens), 0)
    in_first = number == routes[0:1]
    in_second = number == routes[1:2]
    hits = jnp.where(in_first, 1.0, 0.0) + jnp.where(in_second, 1.0, 0.0)
    row = lax.broadcasted_iota(jnp.int32, (tokens, tokens), 0)
    col = lax.broadcasted_iota(jnp.int32, (tokens, tokens), 1)
    earlier = jnp.where(row < col, 1.0, 0.0).astype(BF16)
    rank = dot(hits.astype(BF16), earlier, ((1,), (0,)))
    weight_ref[...] = jnp.where(in_first, first, 0.0) + jnp.where(in_second, second, 0.0)
    rank_ref[...] = jnp.where(hits > 0.0, rank, -1.0)
    place = lax.broadcasted_iota(jnp.int32, (capacity, tokens), 0).astype(F32)

    def box(hop):
        return remote(
            outbox.at[hop], joined_ref.at[me, :, cols(0)], box_send.at[hop], box_recv.at[hop], ep=(me + hop) % ep_size
        )

    for hop in list(range(1, ep_size)) + [0]:
        expert = (me + hop) % ep_size
        same = place == rank_ref[pl.ds(expert, 1), :]
        pick_ref[expert] = jnp.where(same, weight_ref[pl.ds(expert, 1), :], 0.0).astype(BF16)
        chosen = dot(jnp.where(same, 1.0, 0.0).astype(BF16), normed, ((1,), (0,))).astype(BF16)
        if hop:
            outbox[hop] = chosen
            box(hop).start()
        else:
            joined_ref[me, :, cols(0)] = chosen

    def passing(part, bit, hop):
        at = joined_ref.at[(me + ep_size - hop) % ep_size, :, cols(part)]
        return remote(at, at, ag_send.at[part + bit, hop], ag_recv.at[part + bit, hop], tp=flip(lane, bit))

    bits = [1 << i for i in range(tp_size.bit_length() - 1)][::-1]
    passing(0, bits[0], 0).start()

    tap_col[...] = upright(tapx_ref[...])
    tapb_col[...] = upright(tapb_ref[...])
    tapc_col[...] = upright(tapc_ref[...])
    step, cum, cum_col = prefix_decays(dt_ref, rate_ref)
    step_ref[...] = step
    cum_ref[...] = cum
    reach_ref[...] = jnp.broadcast_to(jnp.exp(cum[:, length - 1 :]), reach_ref.shape)
    for head in range(heads):
        col_ref[head] = jnp.broadcast_to(cum_col[:, head : head + 1], (length, LANES))

    @pl.when(me > 0)
    def _():
        for copy in rims:
            copy.wait_recv()

    group = pl.ds(pl.multiple_of(lane * heads // (HEADS // GROUPS) * NSTATE, NSTATE), NSTATE)
    b_conv = conv_rows(b_ref[group, :], brim[group, :], tapb_col[group, :]).astype(BF16)
    c_conv = conv_rows(c_ref[group, :], crim[group, :], tapc_col[group, :]).astype(BF16)
    bconv_ref[...] = b_conv
    conv_ref[...] = c_conv
    score_ref[...] = dot(b_conv, c_conv, ((0,), (0,)))
    brow = lax.broadcasted_iota(jnp.int32, (BLOCK, BLOCK), 0)
    bcol = lax.broadcasted_iota(jnp.int32, (BLOCK, BLOCK), 1)
    causal = brow <= bcol

    def one(head, carry):
        rows = pl.ds(pl.multiple_of(head * HEAD_DIM, HEAD_DIM), HEAD_DIM)
        x = conv_rows(x_ref[rows, :], xrim[rows, :], tap_col[rows, :])
        own = cum_ref[pl.ds(head, 1), :]
        xs = x * step_ref[pl.ds(head, 1), :]
        tail = xs * jnp.exp(own[:, length - 1 :] - own)
        state_ref[rows, :] = dot(tail.astype(BF16), bconv_ref[...], ((1,), (1,)))
        xs = xs.astype(BF16)
        for target in range(length // BLOCK):
            at = slice(target * BLOCK, (target + 1) * BLOCK)
            pieces = []
            for source in range(target + 1):
                of = slice(source * BLOCK, (source + 1) * BLOCK)
                gap = own[:, at] - col_ref[head, of, :]
                if source == target:
                    gap = jnp.where(causal, gap, -jnp.inf)
                pieces.append((score_ref[of, at] * jnp.exp(gap)).astype(BF16))
            mask = pieces[0] if target == 0 else jnp.concatenate(pieces, axis=0)
            y_ref[rows, at] = dot(xs[:, : (target + 1) * BLOCK], mask, ((1,), (0,)))
        return carry

    lax.fori_loop(0, heads * 3 // 4, one, 0)
    for hop in range(1, ep_size):
        if hop == ep_size // 2:
            lax.fori_loop(heads * 3 // 4, heads, one, 0)
            chain = Prefix(
                state_ref, reach_ref, out, out_reach, got, got_reach, pre_send, pre_recv, ep_size
            )
            chain.begin(0, 1)
        box(hop).wait_recv()
        passing(0, bits[0], hop).start()
    have = [0]
    for index, bit in enumerate(bits):
        for hop in range(ep_size):
            passing(0, bit, hop).wait_recv()
            for part in have[1:]:
                passing(part, bit, hop).wait_recv()
            if index + 1 < len(bits):
                for part in have + [part + bit for part in have]:
                    passing(part, bits[index + 1], hop).start()
        have = have + [part + bit for part in have]
        if index == 0:
            chain.finish(0, 1, True)
            chain.begin(1, 1)
    chain.finish(1, 1, False)
    have = [0]
    for bit in bits:
        for hop in range(ep_size):
            for part in have:
                passing(part, bit, hop).wait_send()
        have = have + [part + bit for part in have]
    for hop in range(1, ep_size):
        box(hop).wait_send()

    @pl.when(me + 1 < ep_size)
    def _():
        for copy in rims:
            copy.wait_send()


def gather_kernel(
    part_ref, first_ref, first_reach,
    back_ref, state_ref,
    sums, landed, final, reach_ref, out, out_reach, got, got_reach,
    rs_send, rs_recv, box_send, box_recv, pre_send, pre_recv,
    *, ep_size, tp_size, rounds,
):
    me, lane = lax.axis_index("ep"), lax.axis_index("tp")
    width = part_ref.shape[2] // tp_size
    greet(ep_size, tp_size)
    bits = [1 << i for i in range(tp_size.bit_length() - 1)]
    order = list(range(1, ep_size)) + [0]

    def cols(part):
        return pl.ds(pl.multiple_of(flip(lane, part) * width, LANES), width)

    def passing(part, bit, hop):
        chunk = (me + hop) % ep_size
        source = part_ref.at[chunk, :, cols(part)] if bit == 1 else sums.at[part, chunk]
        return remote(source, landed.at[part, chunk], rs_send.at[part, hop], rs_recv.at[part, hop], tp=flip(lane, bit))

    def box(hop):
        return remote(final.at[hop], back_ref.at[me], box_send.at[hop], box_recv.at[hop], ep=(me + hop) % ep_size)

    for hop in order:
        for part in range(1, tp_size, 2):
            passing(part, 1, hop).start()
    state_ref[...] = first_ref[...]
    reach_ref[...] = first_reach[...]
    chain = Prefix(state_ref, reach_ref, out, out_reach, got, got_reach, pre_send, pre_recv, ep_size)
    if rounds:
        chain.begin(0, rounds[0])
    done = 0
    for bit in bits:
        kept = range(0, tp_size, 2 * bit)
        for hop in order:
            chunk = (me + hop) % ep_size
            for part in list(kept)[::-1]:
                passing(part + bit, bit, hop).wait_recv()
                mine = part_ref[chunk, :, cols(part)] if bit == 1 else sums[part, chunk]
                total = (mine.astype(F32) + landed[part + bit, chunk].astype(F32)).astype(BF16)
                if bit < bits[-1]:
                    sums[part, chunk] = total
                    if part & (2 * bit):
                        passing(part, 2 * bit, hop).start()
                elif hop:
                    final[hop] = total
                    box(hop).start()
                else:
                    back_ref[me] = total
        if done < len(rounds):
            chain.finish(done, rounds[done], False)
            done += 1
            if done < len(rounds):
                chain.begin(done, rounds[done])
    while done < len(rounds):
        chain.finish(done, rounds[done], False)
        done += 1
        if done < len(rounds):
            chain.begin(done, rounds[done])
    for hop in range(1, ep_size):
        box(hop).wait_recv()
        box(hop).wait_send()
    for bit in bits:
        for part in range(bit, tp_size, 2 * bit):
            for hop in order:
                passing(part, bit, hop).wait_send()


def close_kernel(y_ref, state_ref, conv_ref, cum_ref, z_ref, gain_ref, out_ref, gain_col):
    heads = cum_ref.shape[0]
    top = lax.broadcasted_iota(jnp.int32, (8, LANES), 0) == 0
    flat = jnp.broadcast_to(gain_ref[...], (8, gain_ref.shape[1]))
    gain_col[...] = dot(flat, jnp.where(top, 1.0, 0.0), ((0,), (0,)), lax.Precision.HIGHEST)

    def one(head, carry):
        rows = pl.ds(pl.multiple_of(head * HEAD_DIM, HEAD_DIM), HEAD_DIM)
        carried = dot(state_ref[rows, :].astype(BF16), conv_ref[...], ((1,), (0,)))
        y = y_ref[rows, :] + carried * jnp.exp(cum_ref[pl.ds(head, 1), :])
        gated = y * silu(z_ref[rows, :].astype(F32))
        scale = lax.rsqrt(jnp.mean(gated * gated, axis=0, keepdims=True) + HEAD_EPS)
        out_ref[rows, :] = (gated * scale * gain_col[rows, 0:1]).astype(BF16)
        return carry

    lax.fori_loop(0, heads, one, 0)


def ffn_kernel(joined, gate_ref, up_ref, down_ref, out_ref, total):
    turn = pl.program_id(0)
    gate = dot(joined[...], gate_ref[0], ((1,), (0,)))
    up = dot(joined[...], up_ref[0], ((1,), (0,)))
    hidden = (silu(gate) * up).astype(BF16)
    partial = dot(hidden, down_ref[0], ((1,), (0,)))

    @pl.when(turn == 0)
    def _():
        total[...] = partial

    @pl.when(turn > 0)
    def _():
        total[...] += partial

    @pl.when(turn == pl.num_programs(0) - 1)
    def _():
        out_ref[...] = total[...].astype(BF16)


def combine_kernel(back_ref, pick_ref, out_ref):
    out_ref[...] = dot(pick_ref[...], back_ref[...], ((0,), (0,))).astype(BF16)


def on_device(
    x_in, z_in, dt_raw, decay_rate, b_in, c_in, conv_x, conv_b, conv_c, head_gain,
    moe_rows, moe_gain, routes, route_logit, w_gate, w_up, w_down,
):
    heads, length = dt_raw.shape
    value_rows = x_in.shape[0]
    taps = conv_x.shape[1]
    tp_size = lax.axis_size("tp")
    ep_size = lax.axis_size("ep")
    tokens, features = moe_rows.shape
    experts = ep_size
    capacity = 2 * tokens * routes.shape[1] // experts
    width = features // tp_size
    slots = experts * capacity
    dma = pltpu.SemaphoreType.DMA
    shape = jax.ShapeDtypeStruct

    def chain(turns):
        return [
            VMEM((turns, value_rows, NSTATE), BF16),
            VMEM((turns, heads, NSTATE), F32),
            VMEM((turns, value_rows, NSTATE), BF16),
            VMEM((turns, heads, NSTATE), F32),
        ]

    joined, pick, y_local, state, reach, c_conv, cum = pl.pallas_call(
        functools.partial(spread_kernel, ep_size=ep_size, tp_size=tp_size),
        out_shape=(
            shape((experts, capacity, features), BF16),
            shape((experts, capacity, tokens), BF16),
            shape((value_rows, length), F32),
            shape((value_rows, NSTATE), F32),
            shape((heads, NSTATE), F32),
            shape((NSTATE, length), BF16),
            shape((heads, length), F32),
        ),
        in_specs=vmem_specs(12),
        out_specs=tuple(vmem_specs(7)),
        scratch_shapes=[
            VMEM((experts, capacity, width), BF16),
            VMEM((experts, tokens), F32),
            VMEM((experts, tokens), F32),
            VMEM((value_rows, LANES), BF16),
            VMEM((b_in.shape[0], LANES), BF16),
            VMEM((c_in.shape[0], LANES), BF16),
            VMEM((value_rows, taps), F32),
            VMEM((b_in.shape[0], taps), F32),
            VMEM((c_in.shape[0], taps), F32),
            VMEM((heads, length), F32),
            VMEM((heads, length, LANES), F32),
            VMEM((length, length), F32),
            VMEM((NSTATE, length), BF16),
        ]
        + chain(2)
        + [
            dma((3,)), dma((3,)), dma((ep_size,)), dma((ep_size,)),
            dma((tp_size, ep_size)), dma((tp_size, ep_size)), dma((2, 2)), dma((2, 2)),
        ],
        compiler_params=pltpu.CompilerParams(collective_id=0, has_side_effects=True, vmem_limit_bytes=48 * 2**20),
        name="spread",
    )(
        moe_rows, moe_gain.reshape(1, features), routes.T, route_logit.T,
        x_in, conv_x.T, b_in, conv_b.T, c_in, conv_c.T, dt_raw, decay_rate.reshape(1, heads),
    )

    hidden_units = w_gate.shape[2]
    tile = hidden_units if hidden_units < 1024 else 256
    partial = pl.pallas_call(
        ffn_kernel,
        grid=(hidden_units // tile,),
        out_shape=shape((slots, features), BF16),
        in_specs=vmem_specs(1)
        + [
            pl.BlockSpec((1, features, tile), lambda i: (0, 0, i)),
            pl.BlockSpec((1, features, tile), lambda i: (0, 0, i)),
            pl.BlockSpec((1, tile, features), lambda i: (0, i, 0)),
        ],
        out_specs=pl.BlockSpec(memory_space=VMEM),
        scratch_shapes=[VMEM((slots, features), F32)],
        compiler_params=pltpu.CompilerParams(dimension_semantics=("arbitrary",), vmem_limit_bytes=48 * 2**20),
        name="ffn",
    )(joined.reshape(slots, features), w_gate, w_up, w_down)

    rounds = []
    steps = 2
    while steps < ep_size - 1:
        rounds.append(steps)
        steps *= 2
    turns = max(1, len(rounds))
    returned, incoming = pl.pallas_call(
        functools.partial(gather_kernel, ep_size=ep_size, tp_size=tp_size, rounds=rounds),
        out_shape=(shape((experts, capacity, width), BF16), shape((value_rows, NSTATE), F32)),
        in_specs=vmem_specs(3),
        out_specs=tuple(vmem_specs(2)),
        scratch_shapes=[
            VMEM((tp_size, experts, capacity, width), BF16),
            VMEM((tp_size, experts, capacity, width), BF16),
            VMEM((experts, capacity, width), BF16),
            VMEM((heads, NSTATE), F32),
        ]
        + chain(turns)
        + [
            dma((tp_size, ep_size)), dma((tp_size, ep_size)), dma((ep_size,)), dma((ep_size,)),
            dma((turns, 2)), dma((turns, 2)),
        ],
        compiler_params=pltpu.CompilerParams(collective_id=1, has_side_effects=True, vmem_limit_bytes=48 * 2**20),
        name="gather",
    )(partial.reshape(experts, capacity, features), state, reach)

    mixed = pl.pallas_call(
        close_kernel,
        out_shape=shape((value_rows, length), BF16),
        in_specs=vmem_specs(6),
        out_specs=pl.BlockSpec(memory_space=VMEM),
        scratch_shapes=[VMEM((value_rows, LANES), F32)],
        name="close",
    )(y_local, incoming, c_conv, cum, z_in, head_gain.reshape(1, value_rows))
    moe_out = pl.pallas_call(
        combine_kernel,
        out_shape=shape((tokens, width), BF16),
        in_specs=vmem_specs(2),
        out_specs=pl.BlockSpec(memory_space=VMEM),
        name="combine",
    )(returned.reshape(slots, width), pick.reshape(slots, tokens))
    return (mixed, moe_out.T)


def solution(mesh):
    return jax.shard_map(
        on_device,
        mesh=mesh,
        in_specs=(
            P("tp", "ep"), P("tp", "ep"), P("tp", "ep"), P("tp"), P(None, "ep"), P(None, "ep"),
            P("tp", None), P(), P(), P("tp"), P("ep", None), P(), P("ep", None), P("ep", None),
            P("ep", None, "tp"), P("ep", None, "tp"), P("ep", "tp", None),
        ),
        out_specs=(P("tp", "ep"), P("tp", "ep")),
        check_vma=False,
    )
```
